32 devices in a mesh: sp: 8 (over z, y), tp: 4 (over x, core).
Axes of the slice: x: 2, y: 2, z: 4, core: 2. Of those that a mesh axis runs over, the one named last changes fastest.
Arguments:
- expert_input: bfloat16 [3072, 2048], P('sp'), may hold values from -6 to 6
- cotangent: bfloat16 [3072, 2048], P('sp'), may hold values from -6 to 6
- routes: int32 [3072, 2], P('sp'), may hold values from 0 to 7, all different within a row; in each aligned block of 384 rows (0 to 383, 384 to 767, ...) at most 144 rows name the same one
- route_weight: float32 [3072, 2], P('sp'), may hold values from 0.2 to 2.5
- expert_gate: bfloat16 [8, 2048, 1024], P('sp', None, 'tp'), may hold values from -0.125 to 0.125
- expert_up: bfloat16 [8, 2048, 1024], P('sp', None, 'tp'), may hold values from -0.125 to 0.125
- expert_down: bfloat16 [8, 1024, 2048], P('sp', 'tp'), may hold values from -0.1875 to 0.1875
- conv_out: bfloat16 [3072, 1024], P('sp', 'tp'), may hold values from -14 to 14
- conv_value: bfloat16 [3072, 1024], P('sp', 'tp'), may hold values from -6 to 6
- conv_gate: bfloat16 [3072, 1024], P('sp', 'tp'), may hold values from -6 to 6
- conv_taps: float32 [31, 1024], P(None, 'tp'), may hold values from -1 to 1
- norm_gain: float32 [1024], P('tp'), may hold values from 0.1 to 1.9
- norm_bias: float32 [1024], P('tp'), may hold values from -3 to 3
- out_weight: bfloat16 [1024, 2048], P('tp'), may hold values from -0.1875 to 0.1875
Outputs:
- gate_grad: float32 [8, 2048, 1024], P('sp', None, 'tp')
- up_grad: float32 [8, 2048, 1024], P('sp', None, 'tp')
- down_grad: float32 [8, 1024, 2048], P('sp', 'tp')
- resid_grad: bfloat16 [3072, 2048], P('sp')
- out_weight_grad: float32 [1024, 2048], P('tp', 'sp')
- value_grad: bfloat16 [3072, 1024], P('sp', 'tp')
- gate_in_grad: bfloat16 [3072, 1024], P('sp', 'tp')
The draws below stay inside these ranges and needn't reach their ends.
Inputs may be any that keep to these rules, and one draw needn't show every extreme that they name: `routes`: each token names 2 different experts. In each aligned block of 384 tokens no expert is named by more than 144 tokens, and in every draw some block has an expert named by exactly 144 tokens.
All inputs are finite; a program needn't handle non-finite values.
Results may differ from the reference program's by a relative error of at most 0.018.
Values may be sent and summed in bfloat16 or wider, within the bound.
A program may use at most 128 MiB of HBM per device.

```python
import math
import jax
import jax.numpy as jnp
import numpy as np
from jax import lax

D = 2048
CW = 1024
FF = 1024
KW = 31
TOP = 2
TOK_DEV = 384
TOKENS = 3072
EXPERTS = 8
CAP = 144
FGROUP = 256
N_SP = 8
N_TP = 4


def draw_conv_out(key, part):
    first_key = jax.random.fold_in(jax.random.fold_in(key, 11), 0)
    column = jnp.arange(CW, dtype=jnp.float32) / CW
    col_scale = 0.3 * jnp.exp(jnp.log(10.0) * column)[None, :]
    values = jnp.clip(jax.random.normal(first_key, (TOKENS, CW), jnp.float32), -4.0, 4.0) * col_scale
    return values.astype(jnp.bfloat16)


def spiked(array, rng, source, target, parts, factor):
    def block_of(axis_at):
        return (jnp.arange(array.shape[axis_at]) // (array.shape[axis_at] // parts)).reshape((-1,) + (1,) * (array.ndim - 1 - axis_at))

    near = jax.random.permutation(rng, parts)[block_of(target)]
    other_side = (block_of(target) + parts // 2) % parts
    return jnp.where((block_of(source) == near) | (block_of(source) == other_side), factor * array, array)


def levels(stream_key, dims, pieces, low, largest):
    loudness, own = 1.0, jax.random.fold_in(stream_key, 6)
    for position, parts in pieces:
        steps = jnp.exp(jax.random.uniform(jax.random.fold_in(own, position), (parts,), jnp.float32, low / len(pieces), largest / len(pieces)))
        loudness = loudness * jnp.repeat(steps, dims[position] // parts).reshape([-1 if axis == position else 1 for axis in range(len(dims))])
    return loudness


def assign_block(rng, own, number, rows, number_of, top, most, skew):
    order = jax.random.permutation(rng, number_of)
    crowded, usual = load_shares(number_of, rows * top, most, skew, True), load_shares(number_of, rows * top, most, skew, False)
    places = jnp.arange(number_of)

    def named(tallies, rotation):
        used = int((tallies > 0).sum())
        fixed = max(1, used // 4)
        moved = fixed + (places - fixed + rotation * (used - fixed)) % max(1, number_of - fixed)
        return jnp.zeros((number_of,), jnp.int32).at[order[jnp.where(places < fixed, places, moved)]].set(jnp.asarray(tallies, jnp.int32))

    tallies = jnp.where(number % 4 == 0, named(crowded, number // 4), named(usual, number - number // 4 - 1))
    mixed = jax.random.permutation(jax.random.fold_in(own, 3), number_of)
    donor, taker = mixed[0:number_of // 2 * 2:2], mixed[1:number_of // 2 * 2:2]
    slack = jnp.minimum(tallies[donor] - 1, most - tallies[taker]) // 2
    slack = jnp.where((donor == order[0]) | (taker == order[0]) | (tallies[taker] == 0), 0, jnp.maximum(slack, 0))
    moved = jax.random.randint(jax.random.fold_in(own, 4), (number_of // 2,), 0, 1 << 20) % (slack + 1)
    tallies = tallies.at[donor].add(-moved).at[taker].add(moved)
    items = jnp.searchsorted(jnp.cumsum(tallies), jnp.arange(rows * top), side="right").astype(jnp.int32)
    grid = items.reshape(top, rows).T
    grid = grid[jax.random.permutation(jax.random.fold_in(own, 1), rows)]
    rotation = jax.random.randint(jax.random.fold_in(own, 2), (rows, 1), 0, top)
    return jnp.take_along_axis(grid, (jnp.arange(top)[None, :] + rotation) % top, axis=1)


def load_shares(count, total, bound, slope, full):
    loads = [(1 << 20) // math.isqrt(grade ** slope) + 1 for grade in range(1, count + 1)]
    largest = bound if full else min(bound, max(-(-total // count), total * loads[0] // sum(loads)))
    least = 1 if total - largest >= count - 1 else 0
    holding, rest = [largest] + [least] * (count - 1), total - largest - least * (count - 1)
    while rest > 0:
        free = [i for i in range(1, count) if holding[i] < largest] or [i for i in range(1, count) if holding[i] < bound]
        mass, left = sum([loads[i] for i in free]), rest
        for i in free:
            addition = min(bound - holding[i], max(1, left * loads[i] // mass), rest)
            holding[i] = holding[i] + addition
            rest = rest - addition
    return np.array(holding)


def centred(rng, shape, width, most, pieces=(), kind=jnp.bfloat16):
    gain = levels(rng, shape, pieces, -0.22, 0.18) if pieces else 1.0
    entries = jax.random.normal(rng, shape, jnp.float32) * width * gain
    return jnp.minimum(jnp.maximum(entries, -most), most).astype(kind)


def noise_with(rng, shape, scale, limit, pieces, heavy, kind=jnp.bfloat16):
    entries = scale * jax.random.normal(rng, shape, jnp.float32)
    if pieces:
        entries = entries * levels(rng, shape, pieces, -0.22, 0.18)
    return jnp.clip(spiked(entries, jax.random.fold_in(rng, 3), *heavy), -limit, limit).astype(kind)


def setup_inputs(seed: int = 0) -> dict:
    key_list = jax.random.split(jax.random.key(seed), 15)
    expert_input = centred(key_list[0], (TOKENS, D), 1.0, 6.0, ((0, 8),))
    cotangent = noise_with(key_list[1], (TOKENS, D), 1.0, 6.0, ((0, 8),), (0, 1, 8, 2.0))
    routes_keys = jax.random.split(jax.random.fold_in(key_list[2], 1), TOKENS // TOK_DEV)
    routes_turns = jax.random.permutation(jax.random.fold_in(key_list[2], 3), TOKENS // TOK_DEV)
    routes = jax.vmap(lambda own, number: assign_block(jax.random.fold_in(key_list[2], 2), own, number, TOK_DEV, EXPERTS, TOP, CAP, 1))(routes_keys, routes_turns).reshape((TOKENS, TOP))
    route_weight = jnp.clip(jnp.exp(math.log(2.5) - 2.5257286 * jax.random.uniform(key_list[3], (TOKENS, TOP), jnp.float32) ** levels(key_list[3], (TOKENS, TOP), ((0, 8),), -0.2, 0.2)), 0.2, 2.5)
    expert_gate = centred(key_list[4], (EXPERTS, D, FF), D ** -0.5, 0.125, ((0, 8), (2, 4)))
    expert_up = centred(key_list[5], (EXPERTS, D, FF), D ** -0.5, 0.125, ((0, 8), (2, 4)))
    expert_down = centred(key_list[6], (EXPERTS, FF, D), FF ** -0.5, 0.1875, ((0, 8), (1, 4)))
    conv_out = draw_conv_out(jax.random.fold_in(key_list[14], 71), 0)
    conv_value = centred(key_list[8], (TOKENS, CW), 1.0, 6.0, ((0, 8), (1, 4)))
    conv_gate = centred(key_list[9], (TOKENS, CW), 1.0, 6.0, ((0, 8), (1, 4)))
    conv_taps = centred(key_list[10], (KW, CW), KW ** -0.5, 1.0, ((1, 4),), jnp.float32)
    norm_gain = jnp.clip(1.0 + 0.18 * jax.random.normal(key_list[11], (CW,), jnp.float32), 0.1, 1.9)
    norm_bias = centred(key_list[12], (CW,), 0.5, 3.0, ((0, 4),), jnp.float32)
    out_weight = centred(key_list[13], (CW, D), CW ** -0.5, 0.1875, ((0, 4),))
    return {"expert_input": expert_input, "cotangent": cotangent, "routes": routes, "route_weight": route_weight, "expert_gate": expert_gate, "expert_up": expert_up, "expert_down": expert_down, "conv_out": conv_out, "conv_value": conv_value, "conv_gate": conv_gate, "conv_taps": conv_taps, "norm_gain": norm_gain, "norm_bias": norm_bias, "out_weight": out_weight}


norm_eps = 1e-06

def build_slots(block_routes):
    assigns = block_routes.shape[0] * block_routes.shape[1]
    flat_routes = block_routes.reshape(assigns)
    onehot = (flat_routes[:, None] == jnp.arange(EXPERTS, dtype=jnp.int32)[None, :]).astype(jnp.int32)
    slot_rank = lax.optimization_barrier(jnp.sum((jnp.cumsum(onehot, axis=0) - onehot) * onehot, axis=1))
    target = flat_routes * CAP + slot_rank
    return jnp.full((EXPERTS * CAP,), assigns, jnp.int32).at[target].set(jnp.arange(assigns, dtype=jnp.int32))

def reference(expert_input, cotangent, routes, route_weight, expert_gate, expert_up, expert_down, conv_out, conv_value, conv_gate, conv_taps, norm_gain, norm_bias, out_weight):
    block_assigns = TOK_DEV * TOP
    slot_sets = jax.vmap(build_slots)(routes.reshape(N_SP, TOK_DEV, TOP))
    offsets = (jnp.arange(N_SP, dtype=jnp.int32) * block_assigns)[:, None]
    global_ids = jnp.where(slot_sets == block_assigns, TOKENS * TOP, slot_sets + offsets).astype(jnp.int32)
    expert_ids = global_ids.reshape(N_SP, EXPERTS, CAP).transpose(1, 0, 2).reshape(EXPERTS, N_SP * CAP)
    scaled = (cotangent.astype(jnp.float32)[:, None, :] * route_weight[:, :, None]).astype(jnp.bfloat16)
    padded_cot = jnp.concatenate([scaled.reshape(TOKENS * TOP, D), jnp.zeros((1, D), jnp.bfloat16)], axis=0)
    padded_in = jnp.concatenate([expert_input, jnp.zeros((1, D), jnp.bfloat16)], axis=0)

    def expert_step(routed, inputs):
        slot_ids, w_gate, w_up, w_down = inputs
        tokens_of = slot_ids // TOP
        slot_rows = padded_in[tokens_of]
        slot_cots = padded_cot[slot_ids]
        pre_gate = jnp.dot(slot_rows, w_gate, preferred_element_type=jnp.float32)
        pre_up = jnp.dot(slot_rows, w_up, preferred_element_type=jnp.float32)
        gate_sig = jax.nn.sigmoid(pre_gate)
        gate_act = pre_gate * gate_sig
        hidden = (gate_act * pre_up).astype(jnp.bfloat16)
        hidden_grad = jnp.dot(slot_cots, w_down.T, preferred_element_type=jnp.float32)
        down_part = jnp.dot(hidden.T, slot_cots, preferred_element_type=jnp.float32)
        gate_pre = (hidden_grad * pre_up * gate_sig * (1.0 + pre_gate * (1.0 - gate_sig))).astype(jnp.bfloat16)
        up_pre = (hidden_grad * gate_act).astype(jnp.bfloat16)
        gate_part = jnp.dot(slot_rows.T, gate_pre, preferred_element_type=jnp.float32)
        up_part = jnp.dot(slot_rows.T, up_pre, preferred_element_type=jnp.float32)
        slot_grad = jnp.zeros((slot_rows.shape[0], D), jnp.float32)
        for group_idx in range(N_TP):
            group_lo = group_idx * FGROUP
            group_hi = group_lo + FGROUP
            group_part = jnp.dot(gate_pre[:, group_lo:group_hi], w_gate[:, group_lo:group_hi].T, preferred_element_type=jnp.float32)
            group_part = group_part + jnp.dot(up_pre[:, group_lo:group_hi], w_up[:, group_lo:group_hi].T, preferred_element_type=jnp.float32)
            slot_grad = slot_grad + lax.optimization_barrier(group_part.astype(jnp.bfloat16)).astype(jnp.float32)
        rounded = lax.optimization_barrier(slot_grad.astype(jnp.bfloat16)).astype(jnp.float32)
        routed = routed.at[tokens_of].add(rounded)
        return (routed, (gate_part, up_part, down_part))
    routed, weight_grads = lax.scan(expert_step, jnp.zeros((TOKENS + 1, D), jnp.float32), (expert_ids, expert_gate, expert_up, expert_down))
    gate_grad, up_grad, down_grad = weight_grads
    resid_grad = (cotangent.astype(jnp.float32) + routed[:TOKENS]).astype(jnp.bfloat16)
    mix_grad = jnp.dot(resid_grad, out_weight.T, preferred_element_type=jnp.float32)
    conv_vals = conv_out.astype(jnp.float32)
    row_mean = lax.optimization_barrier(jnp.mean(conv_vals, axis=1, keepdims=True))
    row_var = lax.optimization_barrier(jnp.mean((conv_vals - row_mean) ** 2, axis=1, keepdims=True))
    row_rstd = lax.rsqrt(row_var + norm_eps)
    normed = (conv_vals - row_mean) * row_rstd
    norm_pre = normed * norm_gain[None, :] + norm_bias[None, :]
    norm_sig = jax.nn.sigmoid(norm_pre)
    conv_act = (norm_pre * norm_sig).astype(jnp.bfloat16)
    out_weight_grad = jnp.dot(conv_act.T, resid_grad, preferred_element_type=jnp.float32)
    norm_grad = mix_grad * norm_sig * (1.0 + norm_pre * (1.0 - norm_sig)) * norm_gain[None, :]
    grad_mean = lax.optimization_barrier(jnp.mean(norm_grad, axis=1, keepdims=True))
    grad_dot = lax.optimization_barrier(jnp.mean(norm_grad * normed, axis=1, keepdims=True))
    conv_grad = row_rstd * (norm_grad - grad_mean - normed * grad_dot)
    extended = jnp.concatenate([conv_grad, jnp.zeros((KW - 1, CW), jnp.float32)], axis=0)
    glu_grad = jnp.zeros((TOKENS, CW), jnp.float32)
    for lag_index in range(KW):
        begin = KW - 1 - lag_index
        glu_grad = glu_grad + conv_taps[lag_index][None, :] * extended[begin:begin + TOKENS]
    gate_sig = jax.nn.sigmoid(conv_gate.astype(jnp.float32))
    value_grad = (glu_grad * gate_sig).astype(jnp.bfloat16)
    gate_in_grad = (glu_grad * conv_value.astype(jnp.float32) * gate_sig * (1.0 - gate_sig)).astype(jnp.bfloat16)
    return (gate_grad, up_grad, down_grad, resid_grad, out_weight_grad, value_grad, gate_in_grad)
```

```python
import functools

import jax
import jax.numpy as jnp
from jax import lax
from jax.experimental import pallas as pl
from jax.experimental.pallas import tpu as pltpu
from jax.sharding import PartitionSpec as P

norm_eps = 1e-06
MESH = pl.DeviceIdType.MESH
bf16 = jnp.bfloat16
f32 = jnp.float32


def doublings(count):
    steps, step = [], 1
    while step < count:
        steps.append(step)
        step *= 2
    return steps


def remote(source, target, send_sem, recv_sem, peer):
    return pltpu.make_async_remote_copy(
        src_ref=source,
        dst_ref=target,
        send_sem=send_sem,
        recv_sem=recv_sem,
        device_id=peer,
        device_id_type=MESH,
    )


def two_rows(first, second):
    lane = lax.broadcasted_iota(jnp.int32, (first.shape[0], 128), 1)
    tile = jnp.where(lane == 0, first, jnp.where(lane == 1, second, 0.0))
    return tile.T[:8]


def share_sums(held_ref, send_sem, recv_sem, me_s, me_t, tp):
    copies = [
        remote(
            held_ref.at[0], held_ref.at[q], send_sem.at[q], recv_sem.at[q], (me_s, me_t ^ q)
        )
        for q in range(1, tp)
    ]
    for copy in copies:
        copy.start()
    return copies


def summed(held_ref, copies):
    value = held_ref[0]
    for q, copy in enumerate(copies, 1):
        copy.wait_recv()
        value = value + held_ref[q]
    return value


def peers_of(me_s, me_t, sp, tp):
    return [(me_s ^ d, me_t) for d in range(1, sp)] + [(me_s, me_t ^ q) for q in range(1, tp)]


def greet(peers):
    barrier = pltpu.get_barrier_semaphore()
    for peer in peers:
        pl.semaphore_signal(barrier, inc=1, device_id=peer, device_id_type=MESH)
    return barrier


def near_blocks(sp):
    return min(4, max(1, sp // 2))


def send_order(sp):
    close = list(range(1, near_blocks(sp)))
    apart = list(range(near_blocks(sp), sp))
    order = []
    for i in range(max(len(close), len(apart))):
        order += close[i : i + 1] + apart[i : i + 1]
    return order


def dot(left, right, contract):
    return lax.dot_general(left, right, (contract, ((), ())), preferred_element_type=f32)


def step_kernel(sp, tp, *refs):
    (routes_ref, weights_ref, gain_ref, bias_ref) = refs[:4]
    sources = refs[4:14]
    (resid_ref, gate_out, up_out, down_out) = refs[14:18]
    (weight_out, value_out, glu_out) = refs[18:21]
    loaded = refs[21:31]
    (x_ref, cot_ref, conv_ref, gate_ref, up_ref) = loaded[:5]
    (down_ref, mixer_ref, value_ref, sluice_ref, taps_ref) = loaded[5:]
    (load_sem, pick_ref, packet_ref, in_ref, hid_ref, pre_ref, part_ref, got_ref) = refs[31:39]
    (back_ref, acc_ref, second_ref, send_sem, recv_sem) = refs[39:44]
    (got_send, got_recv, back_send, back_recv, join_send, join_recv) = refs[44:50]
    (stat_ref, stat_send, stat_recv, mean_ref, mean_send, mean_recv) = refs[50:56]
    (normed_ref, slope_ref, act_ref, mix_ref) = refs[56:60]
    (proj_ref, low_ref, near_ref, sum_ref, far_ref, ext_ref, halo_ref) = refs[60:67]
    (near_send, near_recv, far_send, far_recv, halo_send, halo_recv) = refs[67:]

    me_s, me_t = lax.axis_index("sp"), lax.axis_index("tp")
    tok_rows, width = x_ref.shape
    top_count = routes_ref.shape[0]
    local_exp, _, hidden = gate_ref.shape
    capacity = in_ref.shape[3]
    share = width // tp
    steps = doublings(tp)
    depth = len(steps)
    order = send_order(sp)
    close = near_blocks(sp)
    slot = {}
    for k, m in enumerate(steps):
        for q in range(0, tp, 2 * m):
            slot[k, q] = len(slot)

    def cols(q):
        return pl.ds(pl.multiple_of((me_t ^ q) * share, share), share)

    peers = peers_of(me_s, me_t, sp, tp)
    barrier = greet(peers)
    loads = [
        pltpu.make_async_copy(source, target, load_sem.at[i])
        for i, (source, target) in enumerate(zip(sources, loaded))
    ]
    for copy in loads:
        copy.start()

    experts = sp * local_exp
    routes = routes_ref[...]
    route = [routes[k : k + 1, :] for k in range(top_count)]
    expert_at = lax.broadcasted_iota(jnp.int32, (experts, tok_rows), 0)
    chosen = [route[k] == expert_at for k in range(top_count)]
    named = sum(jnp.where(hit, 1.0, 0.0) for hit in chosen).astype(bf16)
    grid = (tok_rows, tok_rows)
    earlier = jnp.where(
        lax.broadcasted_iota(jnp.int32, grid, 0) < lax.broadcasted_iota(jnp.int32, grid, 1),
        1.0,
        0.0,
    ).astype(bf16)
    before = dot(named, earlier, ((1,), (0,)))
    target = []
    for k in range(top_count):
        rank = jnp.sum(jnp.where(chosen[k], before, 0.0), axis=0, keepdims=True)
        target.append(route[k] * capacity + rank.astype(jnp.int32))
    slot_at = lax.broadcasted_iota(jnp.int32, (capacity, tok_rows), 0)

    loads[0].wait()
    loads[1].wait()
    pl.semaphore_wait(barrier, len(peers))
    copies = {}

    def packet(d, quarters, place):
        for e in range(local_exp):
            base = ((me_s ^ d) * local_exp + e) * capacity
            hits = [target[k] == slot_at + base for k in range(top_count)]
            pick = sum(jnp.where(hit, 1.0, 0.0) for hit in hits).astype(bf16)
            pick_ref[d, e] = pick
            scale = sum(
                jnp.sum(
                    jnp.where(hits[k], weights_ref[k : k + 1, :], 0.0), axis=1, keepdims=True
                )
                for k in range(top_count)
            )
            for q in quarters:
                rows = dot(pick, x_ref[:, cols(q)], ((1,), (0,)))
                cots = dot(pick, cot_ref[:, cols(q)], ((1,), (0,))) * scale
                place(q, 0, e)[...] = rows.astype(bf16)
                place(q, 1, e)[...] = cots.astype(bf16)

    def arriving(d):
        return list(range(0, tp, 2)) if d < close else [0]

    def held_packet(d, q):
        return second_ref.at[d, q // 2 - 1] if q else packet_ref.at[d]

    for d in order:
        packet(d, arriving(d), lambda q, a, e: held_packet(d, q).at[a, e])
        for q in arriving(d):
            copy = remote(
                held_packet(d, q),
                in_ref.at[me_s, :, :, :, cols(q)],
                send_sem.at[q, d],
                recv_sem.at[q, d],
                (me_s ^ d, me_t),
            )
            copy.start()
            copies[q, d] = copy

    def forward(d, q, m):
        place = in_ref.at[me_s ^ d, :, :, :, cols(q)]
        copy = remote(
            place, place, send_sem.at[q ^ m, d], recv_sem.at[q ^ m, d], (me_s, me_t ^ m)
        )
        copy.start()
        copies[q ^ m, d] = copy

    def spread(d):
        if d < close:
            for q in range(0, tp, 2):
                copies[q, d].wait_recv()
                if tp > 1:
                    forward(d, q, 1)
        else:
            copies[0, d].wait_recv()
            for m in reversed(steps):
                forward(d, 0, m)

    def relay(d):
        if d >= close:
            for low in reversed(steps[1:]):
                for q in range(low, tp, 2 * low):
                    copies[q, d].wait_recv()
                    for m in reversed(steps):
                        if m < low:
                            forward(d, q, m)

    def give(k, q, d, source):
        m = steps[k]
        place = slot[k, q ^ m]
        copy = remote(
            source,
            got_ref.at[place, me_s ^ d],
            got_send.at[place, d],
            got_recv.at[place, d],
            (me_s, me_t ^ m),
        )
        copy.start()
        copies["got", k, q ^ m, d] = copy

    def compute(d):
        if d:
            for q in range(1, tp, 2):
                copies[q, d].wait_recv()
        at = me_s ^ d
        for e in range(local_exp):
            slot_rows, slot_cots = in_ref[at, 0, e], in_ref[at, 1, e]
            pre_gate = dot(slot_rows, gate_ref[e], ((1,), (0,)))
            pre_up = dot(slot_rows, up_ref[e], ((1,), (0,)))
            hidden_grad = dot(slot_cots, down_ref[e], ((1,), (1,)))
            gate_sig = jax.nn.sigmoid(pre_gate)
            gate_act = pre_gate * gate_sig
            hid_ref[e, at] = (gate_act * pre_up).astype(bf16)
            gate_pre = (
                hidden_grad * pre_up * gate_sig * (1.0 + pre_gate * (1.0 - gate_sig))
            ).astype(bf16)
            up_pre = (hidden_grad * gate_act).astype(bf16)
            pre_ref[e, at, :, 0:hidden] = gate_pre
            pre_ref[e, at, :, hidden : 2 * hidden] = up_pre
            part = dot(gate_pre, gate_ref[e], ((1,), (1,)))
            part = part + dot(up_pre, up_ref[e], ((1,), (1,)))
            part_ref[at, e] = part.astype(bf16)
        for q in range(1, tp, 2):
            give(0, q, d, part_ref.at[at, :, :, cols(q)])

    def total(k, q, d):
        value = part_ref[me_s ^ d, :, :, cols(q)].astype(f32)
        for j in range(k):
            value = value + got_ref[slot[j, q], me_s ^ d].astype(f32)
        return value.astype(bf16)

    def reduce(k, d):
        for q in range(0, tp, 2 * steps[k - 1]):
            copies["got", k - 1, q, d].wait_recv()
        if k < depth:
            m = steps[k]
            for q in range(m, tp, 2 * m):
                held = part_ref.at[me_s ^ d, :, :, cols(q)]
                held[...] = total(k, q, d)
                give(k, q, d, held)
        elif d:
            held = part_ref.at[me_s ^ d, :, :, cols(0)]
            held[...] = total(k, 0, d)
            copy = remote(
                held,
                back_ref.at[me_s],
                back_send.at[d],
                back_recv.at[d],
                (me_s ^ d, me_t),
            )
            copy.start()
            copies["back", d] = copy
        else:
            back_ref[me_s] = total(k, 0, d)

    loads[2].wait()
    conv_vals = conv_ref[...].astype(f32)
    stat_ref[0] = two_rows(
        jnp.sum(conv_vals, axis=1, keepdims=True),
        jnp.sum(conv_vals * conv_vals, axis=1, keepdims=True),
    )
    stat_copies = share_sums(stat_ref, stat_send, stat_recv, me_s, me_t, tp)
    packet(0, range(tp), lambda q, a, e: in_ref.at[me_s, a, e, :, cols(q)])
    for copy in loads[3:6]:
        copy.wait()
    compute(0)

    channels = conv_ref.shape[1] * tp
    totals = summed(stat_ref, stat_copies).T / channels
    row_mean = totals[:, 0:1]
    row_var = jnp.maximum(totals[:, 1:2] - row_mean * row_mean, 0.0)
    row_rstd = lax.rsqrt(row_var + norm_eps)
    normed = (conv_vals - row_mean) * row_rstd
    norm_pre = normed * gain_ref[...] + bias_ref[...]
    norm_sig = jax.nn.sigmoid(norm_pre)
    normed_ref[...] = normed
    act_ref[...] = (norm_pre * norm_sig).astype(bf16)
    slope_ref[...] = norm_sig * (1.0 + norm_pre * (1.0 - norm_sig)) * gain_ref[...]

    for k in range(1, depth + 1):
        reduce(k, 0)

    plan = [(0, spread), (1, relay), (2, compute)]
    plan += [(2 + k, functools.partial(reduce, k)) for k in range(1, depth + 1)]
    for i in range(len(order) + plan[-1][0]):
        for lag, act in plan:
            if 0 <= i - lag < len(order):
                act(order[i - lag])

    def rows_grad(e, left, right, store, clear):
        if capacity % 16 == 0:
            whole = lambda value: value.reshape(sp * capacity, value.shape[-1])
            store(dot(whole(left(slice(None))), whole(right(slice(None))), ((0,), (0,))))
        else:
            clear()

            @pl.loop(0, sp)
            def _(at):
                store(dot(left(at), right(at), ((0,), (0,))))

    for e in range(local_exp):
        adds = capacity % 16 != 0

        def put(ref, value):
            ref[e] = ref[e] + value if adds else value

        def put_both(both):
            put(gate_out, both[:, 0:hidden])
            put(up_out, both[:, hidden : 2 * hidden])

        def zero(*outs):
            for out in outs:
                out[e] = jnp.zeros(out.shape[1:], f32)

        rows_grad(
            e,
            lambda at: in_ref[at, 0, e],
            lambda at: pre_ref[e, at],
            put_both,
            functools.partial(zero, gate_out, up_out),
        )
        rows_grad(
            e,
            lambda at: hid_ref[e, at],
            lambda at: in_ref[at, 1, e],
            functools.partial(put, down_out),
            functools.partial(zero, down_out),
        )

    for copy in loads[6:]:
        copy.wait()
    acc_ref[...] = cot_ref[:, cols(0)].astype(f32)
    for d in [0] + order:
        if d:
            copies["back", d].wait_recv()
        for e in range(local_exp):
            acc_ref[...] += dot(pick_ref[d, e], back_ref[me_s ^ d, e], ((0,), (0,)))
    resid_ref[:, cols(0)] = acc_ref[...].astype(bf16)

    def join(q, m):
        place = resid_ref.at[:, cols(q)]
        copy = remote(
            place, place, join_send.at[q ^ m], join_recv.at[q ^ m], (me_s, me_t ^ m)
        )
        copy.start()
        copies["join", q ^ m] = copy

    for m in reversed(steps):
        join(0, m)

    pairs = sp // 2
    per_quarter = pairs // tp
    own_pair, side = lax.div(me_s, 2), lax.rem(me_s, 2)
    feats = proj_ref.shape[2]
    own_channels = conv_ref.shape[1]

    def pair_copies(p):
        near = remote(
            low_ref.at[p], near_ref.at[p], near_send.at[p], near_recv.at[p], (me_s ^ 1, me_t)
        )
        far = remote(
            sum_ref.at[p],
            far_ref.at[own_pair],
            far_send.at[p],
            far_recv.at[own_pair],
            (2 * p + side, me_t),
        )
        return near, far

    def pairs_in(q):
        return [(me_t ^ q) * per_quarter + j for j in range(per_quarter)]

    def project(q):
        quarter = resid_ref[:, cols(q)]
        projected = dot(quarter, act_ref[...], ((0,), (0,)))
        for j, p in enumerate(pairs_in(q)):
            start = 2 * j * feats
            proj_ref[p] = projected[start : start + 2 * feats].reshape(2, feats, own_channels)
            low_ref[p] = proj_ref[p, 1 - side].astype(bf16)
            pair_copies(p)[0].start()
        mixed = dot(quarter, mixer_ref[:, cols(q)], ((1,), (1,)))
        if q == 0:
            mix_ref[...] = mixed
        else:
            mix_ref[...] += mixed

    def pass_on(q):
        for p in pairs_in(q):
            near, far = pair_copies(p)
            near.wait_recv()

            @pl.when(p != own_pair)
            def _():
                sum_ref[p] = (proj_ref[p, side] + near_ref[p].astype(f32)).astype(bf16)
                far.start()

    forwards = {}
    for low in reversed(steps[1:]):
        for q in range(low, tp, 2 * low):
            forwards[q] = [m for m in reversed(steps) if m < low]
    ready = [0] + [q for q in range(1, tp) if q not in forwards and q in (1,)]
    ready += [q for q in range(1, tp) if q not in ready and q in forwards]
    ready += [q for q in range(1, tp) if q not in ready]
    for i, q in enumerate(ready):
        if q:
            copies["join", q].wait_recv()
            for m in forwards.get(q, []):
                join(q, m)
        project(q)
        if 1 <= i < len(ready) - 1:
            pass_on(ready[i - 1])

    norm_grad = mix_ref[...] * slope_ref[...]
    mean_ref[0] = two_rows(
        jnp.sum(norm_grad, axis=1, keepdims=True),
        jnp.sum(norm_grad * normed_ref[...], axis=1, keepdims=True),
    )
    mean_copies = share_sums(mean_ref, mean_send, mean_recv, me_s, me_t, tp)
    pass_on(ready[-2])
    means = summed(mean_ref, mean_copies).T / channels
    ext_ref[0:tok_rows, :] = row_rstd * (
        norm_grad - means[:, 0:1] - normed_ref[...] * means[:, 1:2]
    )
    halo_rows = halo_ref.shape[0]
    halo = remote(
        ext_ref.at[0:halo_rows, :],
        halo_ref,
        halo_send,
        halo_recv,
        (lax.rem(me_s + sp - 1, sp), me_t),
    )
    halo.start()
    pass_on(ready[-1])

    taps_count = taps_ref.shape[0]
    chunk = 64 if tok_rows % 64 == 0 else tok_rows

    def convolve(start):
        glu_grad = jnp.zeros((chunk, own_channels), f32)
        for lag_index in range(taps_count):
            begin = start + taps_count - 1 - lag_index
            glu_grad = glu_grad + taps_ref[lag_index, :][None, :] * ext_ref[
                begin : begin + chunk, :
            ]
        at = slice(start, start + chunk)
        gate_sig = jax.nn.sigmoid(sluice_ref[at, :].astype(f32))
        value_out[at, :] = (glu_grad * gate_sig).astype(bf16)
        glu_out[at, :] = (
            glu_grad * value_ref[at, :].astype(f32) * gate_sig * (1.0 - gate_sig)
        ).astype(bf16)

    starts = list(range(0, tok_rows, chunk))
    early = [start for start in starts if start + chunk + taps_count - 1 <= tok_rows]
    for start in early:
        convolve(start)
    halo.wait_recv()
    ext_ref[tok_rows : tok_rows + halo_rows, :] = jnp.where(me_s == sp - 1, 0.0, halo_ref[...])
    for start in starts[len(early) :]:
        convolve(start)

    total_grad = proj_ref[own_pair, side] + near_ref[own_pair].astype(f32)
    for x in range(1, pairs):
        other = own_pair ^ x
        remote(
            sum_ref.at[other],
            far_ref.at[other],
            far_send.at[other],
            far_recv.at[other],
            (2 * other + side, me_t),
        ).wait_recv()
        total_grad = total_grad + far_ref[other].astype(f32)
    weight_out[...] = total_grad.T

    for x in range(pairs):
        near, far = pair_copies(own_pair ^ x)
        near.wait_send()
        if x:
            far.wait_send()
    for copy in [halo, *stat_copies, *mean_copies, *copies.values()]:
        copy.wait_send()


def store_kernel(*refs):
    count = len(refs) // 2
    moves = [
        pltpu.make_async_copy(refs[i], refs[count + i], refs[-1].at[i]) for i in range(count)
    ]
    for move in moves:
        move.start()
    for move in moves:
        move.wait()


def run_step(routes, weights, gain, bias, big, sp, tp):
    x, _, conv, gate, up, down = big[:6]
    taps = big[9]
    tok_rows, width = x.shape
    own_channels = conv.shape[1]
    local_exp, _, hidden = gate.shape
    top_count = routes.shape[0]
    capacity = 3 * top_count * tok_rows // (2 * local_exp * sp)
    share = width // tp
    feats = width // sp
    pairs = sp // 2
    halo_rows = -(-(taps.shape[0] - 1) // 8) * 8
    vmem = pl.BlockSpec(memory_space=pltpu.VMEM)
    hbm = pl.BlockSpec(memory_space=pltpu.HBM)
    part = (sp, local_exp, capacity, share)
    kept = (local_exp, sp, capacity)
    rows = (tok_rows, own_channels)
    piece = (pairs, feats, own_channels)
    dma = pltpu.SemaphoreType.DMA
    outs = (
        jax.ShapeDtypeStruct((tok_rows, width), bf16),
        jax.ShapeDtypeStruct(gate.shape, f32),
        jax.ShapeDtypeStruct(up.shape, f32),
        jax.ShapeDtypeStruct(down.shape, f32),
        jax.ShapeDtypeStruct((own_channels, feats), f32),
        jax.ShapeDtypeStruct(rows, bf16),
        jax.ShapeDtypeStruct(rows, bf16),
    )
    results = pl.pallas_call(
        functools.partial(step_kernel, sp, tp),
        out_shape=tuple(pltpu.VMEM(out.shape, out.dtype) for out in outs),
        in_specs=[vmem] * 4 + [hbm] * len(big),
        out_specs=(vmem,) * len(outs),
        scratch_shapes=[
            *[pltpu.VMEM(array.shape, array.dtype) for array in big],
            dma((len(big),)),
            pltpu.VMEM((sp, local_exp, capacity, tok_rows), bf16),
            pltpu.VMEM((sp, 2, local_exp, capacity, share), bf16),
            pltpu.VMEM((sp, 2, local_exp, capacity, width), bf16),
            pltpu.VMEM((*kept, hidden), bf16),
            pltpu.VMEM((*kept, 2 * hidden), bf16),
            pltpu.VMEM((sp, local_exp, capacity, width), bf16),
            pltpu.VMEM((tp - 1, *part), bf16),
            pltpu.VMEM(part, bf16),
            pltpu.VMEM((tok_rows, share), f32),
            pltpu.VMEM((near_blocks(sp), max(1, tp // 2 - 1), 2, local_exp, capacity, share), bf16),
            dma((tp, sp)),
            dma((tp, sp)),
            dma((tp - 1, sp)),
            dma((tp - 1, sp)),
            dma((sp,)),
            dma((sp,)),
            dma((tp,)),
            dma((tp,)),
            pltpu.VMEM((tp, 8, tok_rows), f32),
            dma((tp,)),
            dma((tp,)),
            pltpu.VMEM((tp, 8, tok_rows), f32),
            dma((tp,)),
            dma((tp,)),
            pltpu.VMEM(rows, f32),
            pltpu.VMEM(rows, f32),
            pltpu.VMEM(rows, bf16),
            pltpu.VMEM(rows, f32),
            pltpu.VMEM((pairs, 2, feats, own_channels), f32),
            pltpu.VMEM(piece, bf16),
            pltpu.VMEM(piece, bf16),
            pltpu.VMEM(piece, bf16),
            pltpu.VMEM(piece, bf16),
            pltpu.VMEM((tok_rows + halo_rows, own_channels), f32),
            pltpu.VMEM((halo_rows, own_channels), f32),
            dma((pairs,)),
            dma((pairs,)),
            dma((pairs,)),
            dma((pairs,)),
            dma(()),
            dma(()),
        ],
        compiler_params=pltpu.CompilerParams(
            collective_id=0, has_side_effects=True, vmem_limit_bytes=55 * 1024 * 1024
        ),
    )(routes, weights, gain, bias, *[pltpu.with_memory_space_constraint(a, pltpu.HBM) for a in big])
    return pl.pallas_call(
        store_kernel,
        out_shape=outs,
        in_specs=[vmem] * len(outs),
        out_specs=(hbm,) * len(outs),
        scratch_shapes=[dma((len(outs),))],
        compiler_params=pltpu.CompilerParams(vmem_limit_bytes=4 * 1024 * 1024),
    )(*[pltpu.with_memory_space_constraint(a, pltpu.VMEM) for a in results])


def on_device(
    expert_input,
    cotangent,
    routes,
    route_weight,
    expert_gate,
    expert_up,
    expert_down,
    conv_out,
    conv_value,
    conv_gate,
    conv_taps,
    norm_gain,
    norm_bias,
    out_weight,
):
    big = (
        expert_input,
        cotangent,
        conv_out,
        expert_gate,
        expert_up,
        expert_down,
        out_weight,
        conv_value,
        conv_gate,
        conv_taps,
    )
    resid_grad, gate_grad, up_grad, down_grad, out_weight_grad, value_grad, gate_in_grad = run_step(
        routes.T,
        route_weight.T,
        norm_gain[None, :],
        norm_bias[None, :],
        big,
        lax.axis_size("sp"),
        lax.axis_size("tp"),
    )
    return (gate_grad, up_grad, down_grad, resid_grad, out_weight_grad, value_grad, gate_in_grad)


def solution(mesh):
    return jax.shard_map(
        on_device,
        mesh=mesh,
        in_specs=(
            P("sp", None),
            P("sp", None),
            P("sp", None),
            P("sp", None),
            P("sp", None, "tp"),
            P("sp", None, "tp"),
            P("sp", "tp", None),
            P("sp", "tp"),
            P("sp", "tp"),
            P("sp", "tp"),
            P(None, "tp"),
            P("tp"),
            P("tp"),
            P("tp", None),
        ),
        out_specs=(
            P("sp", None, "tp"),
            P("sp", None, "tp"),
            P("sp", "tp", None),
            P("sp", None),
            P("tp", "sp"),
            P("sp", "tp"),
            P("sp", "tp"),
        ),
        check_vma=False,
    )
```

```python
import functools

import jax
import jax.numpy as jnp
from jax import lax
from jax.experimental import pallas as pl
from jax.experimental.pallas import tpu as pltpu
from jax.sharding import PartitionSpec as P

norm_eps = 1e-06
MESH = pl.DeviceIdType.MESH
bf16 = jnp.bfloat16
f32 = jnp.float32


def doublings(count):
    steps, step = [], 1
    while step < count:
        steps.append(step)
        step *= 2
    return steps


def remote(source, target, send_sem, recv_sem, peer):
    return pltpu.make_async_remote_copy(
        src_ref=source,
        dst_ref=target,
        send_sem=send_sem,
        recv_sem=recv_sem,
        device_id=peer,
        device_id_type=MESH,
    )


def two_rows(first, second):
    lane = lax.broadcasted_iota(jnp.int32, (first.shape[0], 128), 1)
    tile = jnp.where(lane == 0, first, jnp.where(lane == 1, second, 0.0))
    return tile.T[:8]


def share_sums(held_ref, send_sem, recv_sem, me_s, me_t, tp):
    copies = [
        remote(
            held_ref.at[0], held_ref.at[q], send_sem.at[q], recv_sem.at[q], (me_s, me_t ^ q)
        )
        for q in range(1, tp)
    ]
    for copy in copies:
        copy.start()
    return copies


def summed(held_ref, copies):
    value = held_ref[0]
    for q, copy in enumerate(copies, 1):
        copy.wait_recv()
        value = value + held_ref[q]
    return value


def peers_of(me_s, me_t, sp, tp):
    return [(me_s ^ d, me_t) for d in range(1, sp)] + [(me_s, me_t ^ q) for q in range(1, tp)]


def greet(peers):
    barrier = pltpu.get_barrier_semaphore()
    for peer in peers:
        pl.semaphore_signal(barrier, inc=1, device_id=peer, device_id_type=MESH)
    return barrier


def near_blocks(sp):
    return min(4, max(1, sp // 2))


def apart_blocks(sp):
    return list(range(max(1, sp // 2), sp))


def close_blocks(sp):
    return list(range(1, max(1, sp // 2)))


def send_order(sp):
    apart, close = apart_blocks(sp), close_blocks(sp)
    half = len(apart) // 2
    apart = [apart[i // 2 + (i % 2) * half] for i in range(2 * half)] + apart[2 * half :]
    return close[:1] + apart + close[1:][::-1]


def work_order(sp):
    apart, close = apart_blocks(sp), close_blocks(sp)
    return apart[:2] + close[:1] + apart[2:3] + close[2:] + apart[3:] + close[1:2]


def dot(left, right, contract):
    return lax.dot_general(left, right, (contract, ((), ())), preferred_element_type=f32)


def step_kernel(sp, tp, *refs):
    (routes_ref, weights_ref, gain_ref, bias_ref) = refs[:4]
    sources = refs[4:14]
    (resid_ref, gate_out, up_out, down_out) = refs[14:18]
    (weight_out, value_out, glu_out) = refs[18:21]
    loaded = refs[21:30]
    (x_ref, cot_ref, conv_ref, wide_ref) = loaded[:4]
    (down_ref, mixer_ref, value_ref, sluice_ref, taps_ref) = loaded[4:]
    (load_sem, pick_ref, packet_ref, in_ref, hid_ref, pre_ref, part_ref, got_ref) = refs[30:38]
    (back_ref, acc_ref, second_ref, send_sem, recv_sem) = refs[38:43]
    (got_send, got_recv, back_send, back_recv, join_send, join_recv) = refs[43:49]
    (stat_ref, stat_send, stat_recv, mean_ref, mean_send, mean_recv) = refs[49:55]
    (normed_ref, slope_ref, act_ref, mix_ref) = refs[55:59]
    (proj_ref, low_ref, near_ref, sum_ref, far_ref, ext_ref, halo_ref) = refs[59:66]
    (near_send, near_recv, far_send, far_recv, halo_send, halo_recv) = refs[66:]

    me_s, me_t = lax.axis_index("sp"), lax.axis_index("tp")
    tok_rows, width = x_ref.shape
    top_count = routes_ref.shape[0]
    local_exp, _, hidden = gate_out.shape
    places = [x_ref, cot_ref, conv_ref]
    places += [wide_ref.at[:, :, 0:hidden], wide_ref.at[:, :, hidden : 2 * hidden]]
    places += loaded[4:]
    capacity = in_ref.shape[3]
    share = width // tp
    steps = doublings(tp)
    depth = len(steps)
    order = work_order(sp)
    quarter_size = max(1, sp // 4)
    row = lax.div(me_s, quarter_size)
    at_end = (row == 0) | (row == sp // quarter_size - 1)
    flip = jnp.where(at_end, quarter_size if sp >= 4 else 0, 0)

    def turned(d):
        return d ^ flip if d >= max(1, sp // 2) else d

    close = near_blocks(sp)
    slot = {}
    for k, m in enumerate(steps):
        for q in range(0, tp, 2 * m):
            slot[k, q] = len(slot)

    def cols(q):
        return pl.ds(pl.multiple_of((me_t ^ q) * share, share), share)

    peers = peers_of(me_s, me_t, sp, tp)
    barrier = greet(peers)
    loads = [
        pltpu.make_async_copy(source, target, load_sem.at[i])
        for i, (source, target) in enumerate(zip(sources, places))
    ]
    for copy in loads:
        copy.start()

    experts = sp * local_exp
    routes = routes_ref[...]
    route = [routes[k : k + 1, :] for k in range(top_count)]
    expert_at = lax.broadcasted_iota(jnp.int32, (experts, tok_rows), 0)
    chosen = [route[k] == expert_at for k in range(top_count)]
    named = sum(jnp.where(hit, 1.0, 0.0) for hit in chosen).astype(bf16)
    grid = (tok_rows, tok_rows)
    earlier = jnp.where(
        lax.broadcasted_iota(jnp.int32, grid, 0) < lax.broadcasted_iota(jnp.int32, grid, 1),
        1.0,
        0.0,
    ).astype(bf16)
    before = dot(named, earlier, ((1,), (0,)))
    target = []
    for k in range(top_count):
        rank = jnp.sum(jnp.where(chosen[k], before, 0.0), axis=0, keepdims=True)
        target.append(route[k] * capacity + rank.astype(jnp.int32))
    slot_at = lax.broadcasted_iota(jnp.int32, (capacity, tok_rows), 0)

    loads[0].wait()
    loads[1].wait()
    pl.semaphore_wait(barrier, len(peers))
    copies = {}

    def packet(d, quarters, place):
        for e in range(local_exp):
            base = ((me_s ^ d) * local_exp + e) * capacity
            hits = [target[k] == slot_at + base for k in range(top_count)]
            pick = sum(jnp.where(hit, 1.0, 0.0) for hit in hits).astype(bf16)
            pick_ref[d, e] = pick
            scale = sum(
                jnp.sum(
                    jnp.where(hits[k], weights_ref[k : k + 1, :], 0.0), axis=1, keepdims=True
                )
                for k in range(top_count)
            )
            for q in quarters:
                rows = dot(pick, x_ref[:, cols(q)], ((1,), (0,)))
                cots = dot(pick, cot_ref[:, cols(q)], ((1,), (0,))) * scale
                place(q, 0, e)[...] = rows.astype(bf16)
                place(q, 1, e)[...] = cots.astype(bf16)

    def arriving(d):
        return list(range(0, tp, 2)) if d < close else [0]

    def held_packet(d, q):
        return second_ref.at[d, q // 2 - 1] if q else packet_ref.at[d]

    for d in send_order(sp):
        packet(d, arriving(d), lambda q, a, e: held_packet(d, q).at[a, e])
        for q in arriving(d):
            for a in range(2):
                copy = remote(
                    held_packet(d, q).at[a],
                    in_ref.at[me_s, a, :, :, cols(q)],
                    send_sem.at[q, a, d],
                    recv_sem.at[q, a, d],
                    (me_s ^ d, me_t),
                )
                copy.start()
                copies[q, a, d] = copy

    def arrival(q, a, d):
        place = in_ref.at[me_s ^ turned(d), a, :, :, cols(q)]
        sems = (send_sem.at[q, a, turned(d)], recv_sem.at[q, a, turned(d)])
        return remote(place, place, *sems, (me_s, me_t ^ max(steps, default=0)))

    def forward(a, d, q, m):
        at = turned(d)
        place = in_ref.at[me_s ^ at, a, :, :, cols(q)]
        copy = remote(
            place,
            place,
            send_sem.at[q ^ m, a, at],
            recv_sem.at[q ^ m, a, at],
            (me_s, me_t ^ m),
        )
        copy.start()
        copies["on", q ^ m, a, d] = copy

    def spread(a, d):
        if d < close:
            for q in range(0, tp, 2):
                arrival(q, a, d).wait_recv()
                if tp > 1:
                    forward(a, d, q, 1)
        else:
            arrival(0, a, d).wait_recv()
            for m in reversed(steps):
                forward(a, d, 0, m)

    def relay(a, d):
        if d >= close:
            for low in reversed(steps[1:]):
                for q in range(low, tp, 2 * low):
                    arrival(q, a, d).wait_recv()
                    for m in reversed(steps):
                        if m < low:
                            forward(a, d, q, m)

    def give(k, q, d, source):
        m = steps[k]
        place = slot[k, q ^ m]
        copy = remote(
            source,
            got_ref.at[place, me_s ^ turned(d)],
            got_send.at[place, turned(d)],
            got_recv.at[place, turned(d)],
            (me_s, me_t ^ m),
        )
        copy.start()
        copies["got", k, q ^ m, d] = copy

    def compute(d):
        if d:
            for q in range(1, tp, 2):
                for a in range(2):
                    arrival(q, a, d).wait_recv()
        at = me_s ^ turned(d)
        for e in range(local_exp):
            slot_rows, slot_cots = in_ref[at, 0, e], in_ref[at, 1, e]
            pre = dot(slot_rows, wide_ref[e], ((1,), (0,)))
            pre_gate, pre_up = pre[:, 0:hidden], pre[:, hidden : 2 * hidden]
            hidden_grad = dot(slot_cots, down_ref[e], ((1,), (1,)))
            gate_sig = jax.nn.sigmoid(pre_gate)
            gate_act = pre_gate * gate_sig
            hid_ref[e, at] = (gate_act * pre_up).astype(bf16)
            gate_pre = (
                hidden_grad * pre_up * gate_sig * (1.0 + pre_gate * (1.0 - gate_sig))
            ).astype(bf16)
            up_pre = (hidden_grad * gate_act).astype(bf16)
            pre_ref[e, at, :, 0:hidden] = gate_pre
            pre_ref[e, at, :, hidden : 2 * hidden] = up_pre
            both = jnp.concatenate([gate_pre, up_pre], axis=1)
            part_ref[at, e] = dot(both, wide_ref[e], ((1,), (1,))).astype(bf16)
        for q in range(1, tp, 2):
            give(0, q, d, part_ref.at[at, :, :, cols(q)])

    def total(k, q, d):
        value = part_ref[me_s ^ turned(d), :, :, cols(q)].astype(f32)
        for j in range(k):
            value = value + got_ref[slot[j, q], me_s ^ turned(d)].astype(f32)
        return value.astype(bf16)

    def reduce(k, d):
        for q in range(0, tp, 2 * steps[k - 1]):
            copies["got", k - 1, q, d].wait_recv()
        if k < depth:
            m = steps[k]
            for q in range(m, tp, 2 * m):
                held = part_ref.at[me_s ^ turned(d), :, :, cols(q)]
                held[...] = total(k, q, d)
                give(k, q, d, held)
        elif d:
            at = turned(d)
            held = part_ref.at[me_s ^ at, :, :, cols(0)]
            held[...] = total(k, 0, d)
            copy = remote(
                held, back_ref.at[me_s], back_send.at[at], back_recv.at[at], (me_s ^ at, me_t)
            )
            copy.start()
            copies["back", d] = copy
        else:
            back_ref[me_s] = total(k, 0, d)

    loads[2].wait()
    conv_vals = conv_ref[...].astype(f32)
    stat_ref[0] = two_rows(
        jnp.sum(conv_vals, axis=1, keepdims=True),
        jnp.sum(conv_vals * conv_vals, axis=1, keepdims=True),
    )
    stat_copies = share_sums(stat_ref, stat_send, stat_recv, me_s, me_t, tp)
    packet(0, range(tp), lambda q, a, e: in_ref.at[me_s, a, e, :, cols(q)])
    for copy in loads[3:6]:
        copy.wait()
    compute(0)

    channels = conv_ref.shape[1] * tp

    def normalise():
        totals = summed(stat_ref, stat_copies).T / channels
        row_mean = totals[:, 0:1]
        row_var = jnp.maximum(totals[:, 1:2] - row_mean * row_mean, 0.0)
        row_rstd = lax.rsqrt(row_var + norm_eps)
        normed = (conv_ref[...].astype(f32) - row_mean) * row_rstd
        norm_pre = normed * gain_ref[...] + bias_ref[...]
        norm_sig = jax.nn.sigmoid(norm_pre)
        normed_ref[...] = normed
        act_ref[...] = (norm_pre * norm_sig).astype(bf16)
        slope_ref[...] = norm_sig * (1.0 + norm_pre * (1.0 - norm_sig)) * gain_ref[...]
        return row_rstd

    def rest(d):
        for k in range(2, depth + 1):
            reduce(k, d)

    spread0, spread1 = functools.partial(spread, 0), functools.partial(spread, 1)
    relay0, relay1 = functools.partial(relay, 0), functools.partial(relay, 1)
    r1, r2 = functools.partial(reduce, 1), rest
    plan = [(4, r2), (3, r1), (2, compute), (1, relay0), (1, relay1), (0, spread0), (0, spread1)]
    for i in range(len(order) + max(lag for lag, _ in plan)):
        for lag, act in plan:
            if 0 <= i - lag < len(order):
                act(order[i - lag])
        if i == 1:
            row_rstd = normalise()
        if 1 <= i <= depth:
            reduce(i, 0)

    def rows_grad(e, left, right, store, clear):
        if capacity % 16 == 0:
            whole = lambda value: value.reshape(sp * capacity, value.shape[-1])
            store(dot(whole(left(slice(None))), whole(right(slice(None))), ((0,), (0,))))
        else:
            clear()

            @pl.loop(0, sp)
            def _(at):
                store(dot(left(at), right(at), ((0,), (0,))))

    adds = capacity % 16 != 0

    def put(ref, e, value):
        ref[e] = ref[e] + value if adds else value

    def clear(outs, e):
        for out in outs:
            out[e] = jnp.zeros(out.shape[1:], f32)

    def input_side_grads():
        for e in range(local_exp):

            def put_both(both):
                put(gate_out, e, both[:, 0:hidden])
                put(up_out, e, both[:, hidden : 2 * hidden])

            rows_grad(
                e,
                lambda at: in_ref[at, 0, e],
                lambda at: pre_ref[e, at],
                put_both,
                functools.partial(clear, (gate_out, up_out), e),
            )

    def output_side_grads():
        for e in range(local_exp):
            rows_grad(
                e,
                lambda at: hid_ref[e, at],
                lambda at: in_ref[at, 1, e],
                functools.partial(put, down_out, e),
                functools.partial(clear, (down_out,), e),
            )

    for copy in loads[6:]:
        copy.wait()
    acc_ref[...] = cot_ref[:, cols(0)].astype(f32)
    for d in [0] + order:
        if d:
            came = back_ref.at[me_s ^ turned(d)]
            sems = (back_send.at[turned(d)], back_recv.at[turned(d)])
            remote(came, came, *sems, (me_s ^ turned(d), me_t)).wait_recv()
        for e in range(local_exp):
            picked = pick_ref[turned(d), e]
            acc_ref[...] += dot(picked, back_ref[me_s ^ turned(d), e], ((0,), (0,)))
    resid_ref[:, cols(0)] = acc_ref[...].astype(bf16)

    pairs = sp // 2
    per_quarter = pairs // tp
    own_pair, side = lax.div(me_s, 2), lax.rem(me_s, 2)
    feats = proj_ref.shape[2]
    own_channels = conv_ref.shape[1]
    pieces = 2 if per_quarter == 1 and feats % 128 == 0 else 1
    piece_cols = share // pieces

    def piece(q, h):
        offset = (me_t ^ q) * share
        if pieces == 2:
            offset = offset + (side if h else 1 - side) * feats
        return pl.ds(pl.multiple_of(offset, piece_cols), piece_cols)

    def join(q, h, m):
        place = resid_ref.at[:, piece(q, h)]
        copy = remote(
            place, place, join_send.at[q ^ m, h], join_recv.at[q ^ m, h], (me_s, me_t ^ m)
        )
        copy.start()
        copies["join", q ^ m, h] = copy

    for h in range(pieces):
        for m in reversed(steps):
            join(0, h, m)

    def pair_near(p):
        return remote(
            low_ref.at[p], near_ref.at[p], near_send.at[p], near_recv.at[p], (me_s ^ 1, me_t)
        )

    def pair_far(p):
        return remote(
            sum_ref.at[p],
            far_ref.at[own_pair],
            far_send.at[p],
            far_recv.at[own_pair],
            (2 * p + side, me_t),
        )

    def pairs_in(q):
        return [(me_t ^ q) * per_quarter + j for j in range(per_quarter)]

    def project(q, h):
        quarter = resid_ref[:, piece(q, h)]
        projected = dot(quarter, act_ref[...], ((0,), (0,)))
        if pieces == 2:
            p = (me_t ^ q) * per_quarter
            if h:
                proj_ref[p, side] = projected
            else:
                low_ref[p] = projected.astype(bf16)
                pair_near(p).start()
        else:
            for j, p in enumerate(pairs_in(q)):
                start = 2 * j * feats
                both = projected[start : start + 2 * feats]
                proj_ref[p] = both.reshape(2, feats, own_channels)
                low_ref[p] = proj_ref[p, 1 - side].astype(bf16)
                pair_near(p).start()
        mixed = dot(quarter, mixer_ref[:, piece(q, h)], ((1,), (1,)))
        if q == 0 and h == 0:
            mix_ref[...] = mixed
        else:
            mix_ref[...] += mixed

    def pass_on(q):
        for p in pairs_in(q):
            pair_near(p).wait_recv()

            @pl.when(p != own_pair)
            def _():
                sum_ref[p] = (proj_ref[p, side] + near_ref[p].astype(f32)).astype(bf16)
                pair_far(p).start()

    onward = {}
    for low in reversed(steps[1:]):
        for q in range(low, tp, 2 * low):
            onward[q] = [m for m in reversed(steps) if m < low]

    def arrived(q, h):
        copies["join", q, h].wait_recv()
        for m in onward.get(q, []):
            join(q, h, m)

    direct = [q for q in range(1, tp) if q in steps]
    ready = sorted(direct) + [q for q in range(1, tp) if q not in direct]
    quick, slow = ready[:1], ready[1:]
    for h in range(pieces):
        project(0, h)
    for q in quick:
        for h in range(pieces):
            arrived(q, h)
            project(q, h)
    input_side_grads()
    for q in [0] + quick:
        pass_on(q)
    late = [(q, h) for h in range(pieces) for q in slow]
    for q, h in late[:1]:
        arrived(q, h)
        project(q, h)
    output_side_grads()
    for q, h in late[1:]:
        arrived(q, h)
        project(q, h)

    norm_grad = mix_ref[...] * slope_ref[...]
    mean_ref[0] = two_rows(
        jnp.sum(norm_grad, axis=1, keepdims=True),
        jnp.sum(norm_grad * normed_ref[...], axis=1, keepdims=True),
    )
    mean_copies = share_sums(mean_ref, mean_send, mean_recv, me_s, me_t, tp)
    for q in slow:
        pass_on(q)
    means = summed(mean_ref, mean_copies).T / channels
    ext_ref[0:tok_rows, :] = row_rstd * (
        norm_grad - means[:, 0:1] - normed_ref[...] * means[:, 1:2]
    )
    halo_rows = halo_ref.shape[0]
    halo = remote(
        ext_ref.at[0:halo_rows, :],
        halo_ref,
        halo_send,
        halo_recv,
        (lax.rem(me_s + sp - 1, sp), me_t),
    )
    halo.start()

    taps_count = taps_ref.shape[0]
    chunk = 64 if tok_rows % 64 == 0 else tok_rows

    def convolve(start):
        glu_grad = jnp.zeros((chunk, own_channels), f32)
        for lag_index in range(taps_count):
            begin = start + taps_count - 1 - lag_index
            glu_grad = glu_grad + taps_ref[lag_index, :][None, :] * ext_ref[
                begin : begin + chunk, :
            ]
        at = slice(start, start + chunk)
        gate_sig = jax.nn.sigmoid(sluice_ref[at, :].astype(f32))
        value_out[at, :] = (glu_grad * gate_sig).astype(bf16)
        glu_out[at, :] = (
            glu_grad * value_ref[at, :].astype(f32) * gate_sig * (1.0 - gate_sig)
        ).astype(bf16)

    starts = list(range(0, tok_rows, chunk))
    early = [start for start in starts if start + chunk + taps_count - 1 <= tok_rows]
    for start in early:
        convolve(start)
    halo.wait_recv()
    ext_ref[tok_rows : tok_rows + halo_rows, :] = jnp.where(me_s == sp - 1, 0.0, halo_ref[...])
    for start in starts[len(early) :]:
        convolve(start)

    total_grad = proj_ref[own_pair, side] + near_ref[own_pair].astype(f32)
    for x in range(1, pairs):
        other = own_pair ^ x
        remote(
            sum_ref.at[other],
            far_ref.at[other],
            far_send.at[other],
            far_recv.at[other],
            (2 * other + side, me_t),
        ).wait_recv()
        total_grad = total_grad + far_ref[other].astype(f32)
    weight_out[...] = total_grad.T

    for x in range(pairs):
        pair_near(own_pair ^ x).wait_send()
        if x:
            pair_far(own_pair ^ x).wait_send()
    for copy in [halo, *stat_copies, *mean_copies, *copies.values()]:
        copy.wait_send()


def store_kernel(*refs):
    count = len(refs) // 2
    moves = [
        pltpu.make_async_copy(refs[i], refs[count + i], refs[-1].at[i]) for i in range(count)
    ]
    for move in moves:
        move.start()
    for move in moves:
        move.wait()


def run_step(routes, weights, gain, bias, big, sp, tp):
    x, _, conv, gate, up, down = big[:6]
    taps = big[9]
    tok_rows, width = x.shape
    own_channels = conv.shape[1]
    local_exp, _, hidden = gate.shape
    top_count = routes.shape[0]
    capacity = 3 * top_count * tok_rows // (2 * local_exp * sp)
    share = width // tp
    feats = width // sp
    pairs = sp // 2
    halo_rows = -(-(taps.shape[0] - 1) // 8) * 8
    vmem = pl.BlockSpec(memory_space=pltpu.VMEM)
    hbm = pl.BlockSpec(memory_space=pltpu.HBM)
    part = (sp, local_exp, capacity, share)
    kept = (local_exp, sp, capacity)
    rows = (tok_rows, own_channels)
    piece = (pairs, feats, own_channels)
    dma = pltpu.SemaphoreType.DMA
    outs = (
        jax.ShapeDtypeStruct((tok_rows, width), bf16),
        jax.ShapeDtypeStruct(gate.shape, f32),
        jax.ShapeDtypeStruct(up.shape, f32),
        jax.ShapeDtypeStruct(down.shape, f32),
        jax.ShapeDtypeStruct((own_channels, feats), f32),
        jax.ShapeDtypeStruct(rows, bf16),
        jax.ShapeDtypeStruct(rows, bf16),
    )
    results = pl.pallas_call(
        functools.partial(step_kernel, sp, tp),
        out_shape=tuple(pltpu.VMEM(out.shape, out.dtype) for out in outs),
        in_specs=[vmem] * 4 + [hbm] * len(big),
        out_specs=(vmem,) * len(outs),
        scratch_shapes=[
            *[pltpu.VMEM(array.shape, array.dtype) for array in big[:3]],
            pltpu.VMEM((local_exp, width, 2 * hidden), bf16),
            *[pltpu.VMEM(array.shape, array.dtype) for array in big[5:]],
            dma((len(big),)),
            pltpu.VMEM((sp, local_exp, capacity, tok_rows), bf16),
            pltpu.VMEM((sp, 2, local_exp, capacity, share), bf16),
            pltpu.VMEM((sp, 2, local_exp, capacity, width), bf16),
            pltpu.VMEM((*kept, hidden), bf16),
            pltpu.VMEM((*kept, 2 * hidden), bf16),
            pltpu.VMEM((sp, local_exp, capacity, width), bf16),
            pltpu.VMEM((tp - 1, *part), bf16),
            pltpu.VMEM(part, bf16),
            pltpu.VMEM((tok_rows, share), f32),
            pltpu.VMEM((near_blocks(sp), max(1, tp // 2 - 1), 2, local_exp, capacity, share), bf16),
            dma((tp, 2, sp)),
            dma((tp, 2, sp)),
            dma((tp - 1, sp)),
            dma((tp - 1, sp)),
            dma((sp,)),
            dma((sp,)),
            dma((tp, 2)),
            dma((tp, 2)),
            pltpu.VMEM((tp, 8, tok_rows), f32),
            dma((tp,)),
            dma((tp,)),
            pltpu.VMEM((tp, 8, tok_rows), f32),
            dma((tp,)),
            dma((tp,)),
            pltpu.VMEM(rows, f32),
            pltpu.VMEM(rows, f32),
            pltpu.VMEM(rows, bf16),
            pltpu.VMEM(rows, f32),
            pltpu.VMEM((pairs, 2, feats, own_channels), f32),
            pltpu.VMEM(piece, bf16),
            pltpu.VMEM(piece, bf16),
            pltpu.VMEM(piece, bf16),
            pltpu.VMEM(piece, bf16),
            pltpu.VMEM((tok_rows + halo_rows, own_channels), f32),
            pltpu.VMEM((halo_rows, own_channels), f32),
            dma((pairs,)),
            dma((pairs,)),
            dma((pairs,)),
            dma((pairs,)),
            dma(()),
            dma(()),
        ],
        compiler_params=pltpu.CompilerParams(
            collective_id=0, has_side_effects=True, vmem_limit_bytes=55 * 1024 * 1024
        ),
    )(routes, weights, gain, bias, *[pltpu.with_memory_space_constraint(a, pltpu.HBM) for a in big])
    return pl.pallas_call(
        store_kernel,
        out_shape=outs,
        in_specs=[vmem] * len(outs),
        out_specs=(hbm,) * len(outs),
        scratch_shapes=[dma((len(outs),))],
        compiler_params=pltpu.CompilerParams(vmem_limit_bytes=4 * 1024 * 1024),
    )(*[pltpu.with_memory_space_constraint(a, pltpu.VMEM) for a in results])


def on_device(
    expert_input,
    cotangent,
    routes,
    route_weight,
    expert_gate,
    expert_up,
    expert_down,
    conv_out,
    conv_value,
    conv_gate,
    conv_taps,
    norm_gain,
    norm_bias,
    out_weight,
):
    big = (
        expert_input,
        cotangent,
        conv_out,
        expert_gate,
        expert_up,
        expert_down,
        out_weight,
        conv_value,
        conv_gate,
        conv_taps,
    )
    resid_grad, gate_grad, up_grad, down_grad, out_weight_grad, value_grad, gate_in_grad = run_step(
        routes.T,
        route_weight.T,
        norm_gain[None, :],
        norm_bias[None, :],
        big,
        lax.axis_size("sp"),
        lax.axis_size("tp"),
    )
    return (gate_grad, up_grad, down_grad, resid_grad, out_weight_grad, value_grad, gate_in_grad)


def solution(mesh):
    return jax.shard_map(
        on_device,
        mesh=mesh,
        in_specs=(
            P("sp", None),
            P("sp", None),
            P("sp", None),
            P("sp", None),
            P("sp", None, "tp"),
            P("sp", None, "tp"),
            P("sp", "tp", None),
            P("sp", "tp"),
            P("sp", "tp"),
            P("sp", "tp"),
            P(None, "tp"),
            P("tp"),
            P("tp"),
            P("tp", None),
        ),
        out_specs=(
            P("sp", None, "tp"),
            P("sp", None, "tp"),
            P("sp", "tp", None),
            P("sp", None),
            P("tp", "sp"),
            P("sp", "tp"),
            P("sp", "tp"),
        ),
        check_vma=False,
    )
```

```python
import functools

import jax
import jax.numpy as jnp
from jax import lax
from jax.experimental import pallas as pl
from jax.experimental.pallas import tpu as pltpu
from jax.sharding import PartitionSpec as P

norm_eps = 1e-06
MESH = pl.DeviceIdType.MESH
bf16 = jnp.bfloat16
f32 = jnp.float32


def doublings(count):
    steps, step = [], 1
    while step < count:
        steps.append(step)
        step *= 2
    return steps


def remote(source, target, send_sem, recv_sem, peer):
    return pltpu.make_async_remote_copy(
        src_ref=source,
        dst_ref=target,
        send_sem=send_sem,
        recv_sem=recv_sem,
        device_id=peer,
        device_id_type=MESH,
    )


def two_rows(first, second):
    lane = lax.broadcasted_iota(jnp.int32, (first.shape[0], 128), 1)
    tile = jnp.where(lane == 0, first, jnp.where(lane == 1, second, 0.0))
    return tile.T[:8]


def share_sums(held_ref, send_sem, recv_sem, me_s, me_t, tp):
    copies = [
        remote(
            held_ref.at[0], held_ref.at[q], send_sem.at[q], recv_sem.at[q], (me_s, me_t ^ q)
        )
        for q in range(1, tp)
    ]
    for copy in copies:
        copy.start()
    return copies


def summed(held_ref, copies):
    value = held_ref[0]
    for q, copy in enumerate(copies, 1):
        copy.wait_recv()
        value = value + held_ref[q]
    return value


def peers_of(me_s, me_t, sp, tp):
    return [(me_s ^ d, me_t) for d in range(1, sp)] + [(me_s, me_t ^ q) for q in range(1, tp)]


def greet(peers):
    barrier = pltpu.get_barrier_semaphore()
    for peer in peers:
        pl.semaphore_signal(barrier, inc=1, device_id=peer, device_id_type=MESH)
    return barrier


def near_blocks(sp):
    return min(4, max(1, sp // 2))


def apart_blocks(sp):
    return list(range(max(1, sp // 2), sp))


def close_blocks(sp):
    return list(range(1, max(1, sp // 2)))


def send_order(sp):
    apart, close = apart_blocks(sp), close_blocks(sp)
    half = len(apart) // 2
    apart = [apart[i // 2 + (i % 2) * half] for i in range(2 * half)] + apart[2 * half :]
    return close[:1] + apart + close[1:][::-1]


def work_order(sp):
    apart, close = apart_blocks(sp), close_blocks(sp)
    return apart[:2] + close[:1] + apart[2:3] + close[2:] + apart[3:] + close[1:2]


def dot(left, right, contract):
    return lax.dot_general(left, right, (contract, ((), ())), preferred_element_type=f32)


def step_kernel(sp, tp, *refs):
    (routes_ref, weights_ref, gain_ref, bias_ref) = refs[:4]
    sources = refs[4:14]
    (resid_ref, gate_out, up_out, down_out) = refs[14:18]
    (weight_out, value_out, glu_out) = refs[18:21]
    loaded = refs[21:30]
    (x_ref, cot_ref, conv_ref, wide_ref) = loaded[:4]
    (down_ref, mixer_ref, value_ref, sluice_ref, taps_ref) = loaded[4:]
    (load_sem, pick_ref, packet_ref, in_ref, hid_ref, pre_ref, part_ref, got_ref) = refs[30:38]
    (back_ref, acc_ref, second_ref, send_sem, recv_sem) = refs[38:43]
    (got_send, got_recv, back_send, back_recv, join_send, join_recv) = refs[43:49]
    (stat_ref, stat_send, stat_recv, mean_ref, mean_send, mean_recv) = refs[49:55]
    (normed_ref, slope_ref, act_ref, mix_ref) = refs[55:59]
    (proj_ref, low_ref, near_ref, sum_ref, far_ref, ext_ref, halo_ref) = refs[59:66]
    (near_send, near_recv, far_send, far_recv, halo_send, halo_recv) = refs[66:]

    me_s, me_t = lax.axis_index("sp"), lax.axis_index("tp")
    tok_rows, width = x_ref.shape
    top_count = routes_ref.shape[0]
    local_exp, _, hidden = gate_out.shape
    places = [x_ref, cot_ref, conv_ref]
    places += [wide_ref.at[:, :, 0:hidden], wide_ref.at[:, :, hidden : 2 * hidden]]
    places += loaded[4:]
    capacity = in_ref.shape[3]
    share = width // tp
    steps = doublings(tp)
    depth = len(steps)
    order = work_order(sp)
    quarter_size = max(1, sp // 4)
    row = lax.div(me_s, quarter_size)
    at_end = (row == 0) | (row == sp // quarter_size - 1)
    flip = jnp.where(at_end, quarter_size if sp >= 4 else 0, 0)

    def turned(d):
        return d ^ flip if d >= max(1, sp // 2) else d

    close = near_blocks(sp)
    slot = {}
    for k, m in enumerate(steps):
        for q in range(0, tp, 2 * m):
            slot[k, q] = len(slot)

    def cols(q):
        return pl.ds(pl.multiple_of((me_t ^ q) * share, share), share)

    peers = peers_of(me_s, me_t, sp, tp)
    barrier = greet(peers)
    loads = [
        pltpu.make_async_copy(source, target, load_sem.at[i])
        for i, (source, target) in enumerate(zip(sources, places))
    ]
    for copy in loads:
        copy.start()

    experts = sp * local_exp
    routes = routes_ref[...]
    route = [routes[k : k + 1, :] for k in range(top_count)]
    expert_at = lax.broadcasted_iota(jnp.int32, (experts, tok_rows), 0)
    chosen = [route[k] == expert_at for k in range(top_count)]
    named = sum(jnp.where(hit, 1.0, 0.0) for hit in chosen).astype(bf16)
    grid = (tok_rows, tok_rows)
    earlier = jnp.where(
        lax.broadcasted_iota(jnp.int32, grid, 0) < lax.broadcasted_iota(jnp.int32, grid, 1),
        1.0,
        0.0,
    ).astype(bf16)
    before = dot(named, earlier, ((1,), (0,)))
    target = []
    for k in range(top_count):
        rank = jnp.sum(jnp.where(chosen[k], before, 0.0), axis=0, keepdims=True)
        target.append(route[k] * capacity + rank.astype(jnp.int32))
    slot_at = lax.broadcasted_iota(jnp.int32, (capacity, tok_rows), 0)

    loads[0].wait()
    loads[1].wait()
    pl.semaphore_wait(barrier, len(peers))
    copies = {}

    def packet(d, quarters, place):
        for e in range(local_exp):
            base = ((me_s ^ d) * local_exp + e) * capacity
            hits = [target[k] == slot_at + base for k in range(top_count)]
            pick = sum(jnp.where(hit, 1.0, 0.0) for hit in hits).astype(bf16)
            pick_ref[d, e] = pick
            scale = sum(
                jnp.sum(
                    jnp.where(hits[k], weights_ref[k : k + 1, :], 0.0), axis=1, keepdims=True
                )
                for k in range(top_count)
            )
            for q in quarters:
                rows = dot(pick, x_ref[:, cols(q)], ((1,), (0,)))
                cots = dot(pick, cot_ref[:, cols(q)], ((1,), (0,))) * scale
                place(q, 0, e)[...] = rows.astype(bf16)
                place(q, 1, e)[...] = cots.astype(bf16)

    def arriving(d):
        return list(range(0, tp, 2)) if d < close else [0]

    def held_packet(d, q):
        return second_ref.at[d, q // 2 - 1] if q else packet_ref.at[d]

    for d in send_order(sp):
        packet(d, arriving(d), lambda q, a, e: held_packet(d, q).at[a, e])
        for q in arriving(d):
            for a in range(2):
                copy = remote(
                    held_packet(d, q).at[a],
                    in_ref.at[me_s, a, :, :, cols(q)],
                    send_sem.at[q, a, d],
                    recv_sem.at[q, a, d],
                    (me_s ^ d, me_t),
                )
                copy.start()
                copies[q, a, d] = copy

    def arrival(q, a, d):
        place = in_ref.at[me_s ^ turned(d), a, :, :, cols(q)]
        sems = (send_sem.at[q, a, turned(d)], recv_sem.at[q, a, turned(d)])
        return remote(place, place, *sems, (me_s, me_t ^ max(steps, default=0)))

    def forward(a, d, q, m):
        at = turned(d)
        place = in_ref.at[me_s ^ at, a, :, :, cols(q)]
        copy = remote(
            place,
            place,
            send_sem.at[q ^ m, a, at],
            recv_sem.at[q ^ m, a, at],
            (me_s, me_t ^ m),
        )
        copy.start()
        copies["on", q ^ m, a, d] = copy

    def spread(a, d):
        if d < close:
            for q in range(0, tp, 2):
                arrival(q, a, d).wait_recv()
                if tp > 1:
                    forward(a, d, q, 1)
        else:
            arrival(0, a, d).wait_recv()
            for m in reversed(steps):
                forward(a, d, 0, m)

    def relay(a, d):
        if d >= close:
            for low in reversed(steps[1:]):
                for q in range(low, tp, 2 * low):
                    arrival(q, a, d).wait_recv()
                    for m in reversed(steps):
                        if m < low:
                            forward(a, d, q, m)

    def give(k, q, d, source):
        m = steps[k]
        place = slot[k, q ^ m]
        copy = remote(
            source,
            got_ref.at[place, me_s ^ turned(d)],
            got_send.at[place, turned(d)],
            got_recv.at[place, turned(d)],
            (me_s, me_t ^ m),
        )
        copy.start()
        copies["got", k, q ^ m, d] = copy

    def compute(d):
        if d:
            for q in range(1, tp, 2):
                for a in range(2):
                    arrival(q, a, d).wait_recv()
        at = me_s ^ turned(d)
        for e in range(local_exp):
            slot_rows, slot_cots = in_ref[at, 0, e], in_ref[at, 1, e]
            pre = dot(slot_rows, wide_ref[e], ((1,), (0,)))
            pre_gate, pre_up = pre[:, 0:hidden], pre[:, hidden : 2 * hidden]
            hidden_grad = dot(slot_cots, down_ref[e], ((1,), (1,)))
            gate_sig = jax.nn.sigmoid(pre_gate)
            gate_act = pre_gate * gate_sig
            hid_ref[e, at] = (gate_act * pre_up).astype(bf16)
            gate_pre = (
                hidden_grad * pre_up * gate_sig * (1.0 + pre_gate * (1.0 - gate_sig))
            ).astype(bf16)
            up_pre = (hidden_grad * gate_act).astype(bf16)
            pre_ref[e, at, :, 0:hidden] = gate_pre
            pre_ref[e, at, :, hidden : 2 * hidden] = up_pre
            both = jnp.concatenate([gate_pre, up_pre], axis=1)
            part_ref[at, e] = dot(both, wide_ref[e], ((1,), (1,))).astype(bf16)
        for q in range(1, tp, 2):
            give(0, q, d, part_ref.at[at, :, :, cols(q)])

    def total(k, q, d):
        value = part_ref[me_s ^ turned(d), :, :, cols(q)].astype(f32)
        for j in range(k):
            value = value + got_ref[slot[j, q], me_s ^ turned(d)].astype(f32)
        return value.astype(bf16)

    def reduce(k, d):
        for q in range(0, tp, 2 * steps[k - 1]):
            copies["got", k - 1, q, d].wait_recv()
        if k < depth:
            m = steps[k]
            for q in range(m, tp, 2 * m):
                held = part_ref.at[me_s ^ turned(d), :, :, cols(q)]
                held[...] = total(k, q, d)
                give(k, q, d, held)
        elif d:
            at = turned(d)
            held = part_ref.at[me_s ^ at, :, :, cols(0)]
            held[...] = total(k, 0, d)
            copy = remote(
                held, back_ref.at[me_s], back_send.at[at], back_recv.at[at], (me_s ^ at, me_t)
            )
            copy.start()
            copies["back", d] = copy
        else:
            back_ref[me_s] = total(k, 0, d)

    loads[2].wait()
    conv_vals = conv_ref[...].astype(f32)
    stat_ref[0] = two_rows(
        jnp.sum(conv_vals, axis=1, keepdims=True),
        jnp.sum(conv_vals * conv_vals, axis=1, keepdims=True),
    )
    stat_copies = share_sums(stat_ref, stat_send, stat_recv, me_s, me_t, tp)
    packet(0, range(tp), lambda q, a, e: in_ref.at[me_s, a, e, :, cols(q)])
    for copy in loads[3:6]:
        copy.wait()
    compute(0)

    channels = conv_ref.shape[1] * tp

    def normalise():
        totals = summed(stat_ref, stat_copies).T / channels
        row_mean = totals[:, 0:1]
        row_var = jnp.maximum(totals[:, 1:2] - row_mean * row_mean, 0.0)
        row_rstd = lax.rsqrt(row_var + norm_eps)
        normed = (conv_ref[...].astype(f32) - row_mean) * row_rstd
        norm_pre = normed * gain_ref[...] + bias_ref[...]
        norm_sig = jax.nn.sigmoid(norm_pre)
        normed_ref[...] = normed
        act_ref[...] = (norm_pre * norm_sig).astype(bf16)
        slope_ref[...] = norm_sig * (1.0 + norm_pre * (1.0 - norm_sig)) * gain_ref[...]
        return row_rstd

    def rest(d):
        for k in range(2, depth + 1):
            reduce(k, d)

    spread0, spread1 = functools.partial(spread, 0), functools.partial(spread, 1)
    relay0, relay1 = functools.partial(relay, 0), functools.partial(relay, 1)
    r1, r2 = functools.partial(reduce, 1), rest
    plan = [(0, spread0), (1, relay0), (0, spread1), (1, relay1), (2, r1), (1, compute), (3, r2)]
    for i in range(len(order) + max(lag for lag, _ in plan)):
        for lag, act in plan:
            if 0 <= i - lag < len(order):
                act(order[i - lag])
        if i == 1:
            row_rstd = normalise()
        if 1 <= i <= depth:
            reduce(i, 0)

    def rows_grad(e, left, right, store, clear):
        if capacity % 16 == 0:
            whole = lambda value: value.reshape(sp * capacity, value.shape[-1])
            store(dot(whole(left(slice(None))), whole(right(slice(None))), ((0,), (0,))))
        else:
            clear()

            @pl.loop(0, sp)
            def _(at):
                store(dot(left(at), right(at), ((0,), (0,))))

    adds = capacity % 16 != 0

    def put(ref, e, value):
        ref[e] = ref[e] + value if adds else value

    def clear(outs, e):
        for out in outs:
            out[e] = jnp.zeros(out.shape[1:], f32)

    def input_side_grads():
        for e in range(local_exp):

            def put_both(both):
                put(gate_out, e, both[:, 0:hidden])
                put(up_out, e, both[:, hidden : 2 * hidden])

            rows_grad(
                e,
                lambda at: in_ref[at, 0, e],
                lambda at: pre_ref[e, at],
                put_both,
                functools.partial(clear, (gate_out, up_out), e),
            )

    def output_side_grads():
        for e in range(local_exp):
            rows_grad(
                e,
                lambda at: hid_ref[e, at],
                lambda at: in_ref[at, 1, e],
                functools.partial(put, down_out, e),
                functools.partial(clear, (down_out,), e),
            )

    for copy in loads[6:]:
        copy.wait()
    acc_ref[...] = cot_ref[:, cols(0)].astype(f32)
    for d in [0] + order:
        if d:
            came = back_ref.at[me_s ^ turned(d)]
            sems = (back_send.at[turned(d)], back_recv.at[turned(d)])
            remote(came, came, *sems, (me_s ^ turned(d), me_t)).wait_recv()
        for e in range(local_exp):
            picked = pick_ref[turned(d), e]
            acc_ref[...] += dot(picked, back_ref[me_s ^ turned(d), e], ((0,), (0,)))
    resid_ref[:, cols(0)] = acc_ref[...].astype(bf16)

    pairs = sp // 2
    per_quarter = pairs // tp
    own_pair, side = lax.div(me_s, 2), lax.rem(me_s, 2)
    feats = proj_ref.shape[2]
    own_channels = conv_ref.shape[1]
    pieces = 2 if per_quarter == 1 and feats % 128 == 0 else 1
    piece_cols = share // pieces

    def piece(q, h):
        offset = (me_t ^ q) * share
        if pieces == 2:
            offset = offset + (side if h else 1 - side) * feats
        return pl.ds(pl.multiple_of(offset, piece_cols), piece_cols)

    def join(q, h, m):
        place = resid_ref.at[:, piece(q, h)]
        copy = remote(
            place, place, join_send.at[q ^ m, h], join_recv.at[q ^ m, h], (me_s, me_t ^ m)
        )
        copy.start()
        copies["join", q ^ m, h] = copy

    for h in range(pieces):
        for m in reversed(steps):
            join(0, h, m)

    def pair_near(p):
        return remote(
            low_ref.at[p], near_ref.at[p], near_send.at[p], near_recv.at[p], (me_s ^ 1, me_t)
        )

    def pair_far(p):
        return remote(
            sum_ref.at[p],
            far_ref.at[own_pair],
            far_send.at[p],
            far_recv.at[own_pair],
            (2 * p + side, me_t),
        )

    def pairs_in(q):
        return [(me_t ^ q) * per_quarter + j for j in range(per_quarter)]

    def project(q, h):
        quarter = resid_ref[:, piece(q, h)]
        projected = dot(quarter, act_ref[...], ((0,), (0,)))
        if pieces == 2:
            p = (me_t ^ q) * per_quarter
            if h:
                proj_ref[p, side] = projected
            else:
                low_ref[p] = projected.astype(bf16)
                pair_near(p).start()
        else:
            for j, p in enumerate(pairs_in(q)):
                start = 2 * j * feats
                both = projected[start : start + 2 * feats]
                proj_ref[p] = both.reshape(2, feats, own_channels)
                low_ref[p] = proj_ref[p, 1 - side].astype(bf16)
                pair_near(p).start()
        mixed = dot(quarter, mixer_ref[:, piece(q, h)], ((1,), (1,)))
        if q == 0 and h == 0:
            mix_ref[...] = mixed
        else:
            mix_ref[...] += mixed

    def pass_on(q):
        for p in pairs_in(q):
            pair_near(p).wait_recv()

            @pl.when(p != own_pair)
            def _():
                sum_ref[p] = (proj_ref[p, side] + near_ref[p].astype(f32)).astype(bf16)
                pair_far(p).start()

    onward = {}
    for low in reversed(steps[1:]):
        for q in range(low, tp, 2 * low):
            onward[q] = [m for m in reversed(steps) if m < low]

    def arrived(q, h):
        copies["join", q, h].wait_recv()
        for m in onward.get(q, []):
            join(q, h, m)

    direct = [q for q in range(1, tp) if q in steps]
    ready = sorted(direct) + [q for q in range(1, tp) if q not in direct]
    quick, slow = ready[:1], ready[1:]
    for h in range(pieces):
        project(0, h)
    for q in quick:
        for h in range(pieces):
            arrived(q, h)
            project(q, h)
    input_side_grads()
    for q in [0] + quick:
        pass_on(q)
    sent = [key for key in copies if key[0] != "join"]
    for key in sent:
        copies.pop(key).wait_send()
    late = [(q, h) for h in range(pieces) for q in slow]
    for q, h in late[:1]:
        arrived(q, h)
        project(q, h)
    output_side_grads()
    for q, h in late[1:]:
        arrived(q, h)
        project(q, h)

    norm_grad = mix_ref[...] * slope_ref[...]
    mean_ref[0] = two_rows(
        jnp.sum(norm_grad, axis=1, keepdims=True),
        jnp.sum(norm_grad * normed_ref[...], axis=1, keepdims=True),
    )
    mean_copies = share_sums(mean_ref, mean_send, mean_recv, me_s, me_t, tp)
    for q in slow:
        pass_on(q)
    means = summed(mean_ref, mean_copies).T / channels
    ext_ref[0:tok_rows, :] = row_rstd * (
        norm_grad - means[:, 0:1] - normed_ref[...] * means[:, 1:2]
    )
    halo_rows = halo_ref.shape[0]
    halo = remote(
        ext_ref.at[0:halo_rows, :],
        halo_ref,
        halo_send,
        halo_recv,
        (lax.rem(me_s + sp - 1, sp), me_t),
    )
    halo.start()

    taps_count = taps_ref.shape[0]
    chunk = 64 if tok_rows % 64 == 0 else tok_rows

    def convolve(start):
        glu_grad = jnp.zeros((chunk, own_channels), f32)
        for lag_index in range(taps_count):
            begin = start + taps_count - 1 - lag_index
            glu_grad = glu_grad + taps_ref[lag_index, :][None, :] * ext_ref[
                begin : begin + chunk, :
            ]
        at = slice(start, start + chunk)
        gate_sig = jax.nn.sigmoid(sluice_ref[at, :].astype(f32))
        value_out[at, :] = (glu_grad * gate_sig).astype(bf16)
        glu_out[at, :] = (
            glu_grad * value_ref[at, :].astype(f32) * gate_sig * (1.0 - gate_sig)
        ).astype(bf16)

    starts = list(range(0, tok_rows, chunk))
    early = [start for start in starts if start + chunk + taps_count - 1 <= tok_rows]
    for start in early:
        convolve(start)
    halo.wait_recv()
    ext_ref[tok_rows : tok_rows + halo_rows, :] = jnp.where(me_s == sp - 1, 0.0, halo_ref[...])
    for start in starts[len(early) :]:
        convolve(start)

    total_grad = proj_ref[own_pair, side] + near_ref[own_pair].astype(f32)
    for x in range(1, pairs):
        other = own_pair ^ x
        remote(
            sum_ref.at[other],
            far_ref.at[other],
            far_send.at[other],
            far_recv.at[other],
            (2 * other + side, me_t),
        ).wait_recv()
        total_grad = total_grad + far_ref[other].astype(f32)
    weight_out[...] = total_grad.T

    for x in range(pairs):
        pair_near(own_pair ^ x).wait_send()
        if x:
            pair_far(own_pair ^ x).wait_send()
    for copy in [halo, *stat_copies, *mean_copies, *copies.values()]:
        copy.wait_send()


def store_kernel(*refs):
    count = len(refs) // 2
    moves = [
        pltpu.make_async_copy(refs[i], refs[count + i], refs[-1].at[i]) for i in range(count)
    ]
    for move in moves:
        move.start()
    for move in moves:
        move.wait()


def run_step(routes, weights, gain, bias, big, sp, tp):
    x, _, conv, gate, up, down = big[:6]
    taps = big[9]
    tok_rows, width = x.shape
    own_channels = conv.shape[1]
    local_exp, _, hidden = gate.shape
    top_count = routes.shape[0]
    capacity = 3 * top_count * tok_rows // (2 * local_exp * sp)
    share = width // tp
    feats = width // sp
    pairs = sp // 2
    halo_rows = -(-(taps.shape[0] - 1) // 8) * 8
    vmem = pl.BlockSpec(memory_space=pltpu.VMEM)
    hbm = pl.BlockSpec(memory_space=pltpu.HBM)
    part = (sp, local_exp, capacity, share)
    kept = (local_exp, sp, capacity)
    rows = (tok_rows, own_channels)
    piece = (pairs, feats, own_channels)
    dma = pltpu.SemaphoreType.DMA
    outs = (
        jax.ShapeDtypeStruct((tok_rows, width), bf16),
        jax.ShapeDtypeStruct(gate.shape, f32),
        jax.ShapeDtypeStruct(up.shape, f32),
        jax.ShapeDtypeStruct(down.shape, f32),
        jax.ShapeDtypeStruct((own_channels, feats), f32),
        jax.ShapeDtypeStruct(rows, bf16),
        jax.ShapeDtypeStruct(rows, bf16),
    )
    results = pl.pallas_call(
        functools.partial(step_kernel, sp, tp),
        out_shape=tuple(pltpu.VMEM(out.shape, out.dtype) for out in outs),
        in_specs=[vmem] * 4 + [hbm] * len(big),
        out_specs=(vmem,) * len(outs),
        scratch_shapes=[
            *[pltpu.VMEM(array.shape, array.dtype) for array in big[:3]],
            pltpu.VMEM((local_exp, width, 2 * hidden), bf16),
            *[pltpu.VMEM(array.shape, array.dtype) for array in big[5:]],
            dma((len(big),)),
            pltpu.VMEM((sp, local_exp, capacity, tok_rows), bf16),
            pltpu.VMEM((sp, 2, local_exp, capacity, share), bf16),
            pltpu.VMEM((sp, 2, local_exp, capacity, width), bf16),
            pltpu.VMEM((*kept, hidden), bf16),
            pltpu.VMEM((*kept, 2 * hidden), bf16),
            pltpu.VMEM((sp, local_exp, capacity, width), bf16),
            pltpu.VMEM((tp - 1, *part), bf16),
            pltpu.VMEM(part, bf16),
            pltpu.VMEM((tok_rows, share), f32),
            pltpu.VMEM((near_blocks(sp), max(1, tp // 2 - 1), 2, local_exp, capacity, share), bf16),
            dma((tp, 2, sp)),
            dma((tp, 2, sp)),
            dma((tp - 1, sp)),
            dma((tp - 1, sp)),
            dma((sp,)),
            dma((sp,)),
            dma((tp, 2)),
            dma((tp, 2)),
            pltpu.VMEM((tp, 8, tok_rows), f32),
            dma((tp,)),
            dma((tp,)),
            pltpu.VMEM((tp, 8, tok_rows), f32),
            dma((tp,)),
            dma((tp,)),
            pltpu.VMEM(rows, f32),
            pltpu.VMEM(rows, f32),
            pltpu.VMEM(rows, bf16),
            pltpu.VMEM(rows, f32),
            pltpu.VMEM((pairs, 2, feats, own_channels), f32),
            pltpu.VMEM(piece, bf16),
            pltpu.VMEM(piece, bf16),
            pltpu.VMEM(piece, bf16),
            pltpu.VMEM(piece, bf16),
            pltpu.VMEM((tok_rows + halo_rows, own_channels), f32),
            pltpu.VMEM((halo_rows, own_channels), f32),
            dma((pairs,)),
            dma((pairs,)),
            dma((pairs,)),
            dma((pairs,)),
            dma(()),
            dma(()),
        ],
        compiler_params=pltpu.CompilerParams(
            collective_id=0, has_side_effects=True, vmem_limit_bytes=55 * 1024 * 1024
        ),
    )(routes, weights, gain, bias, *[pltpu.with_memory_space_constraint(a, pltpu.HBM) for a in big])
    return pl.pallas_call(
        store_kernel,
        out_shape=outs,
        in_specs=[vmem] * len(outs),
        out_specs=(hbm,) * len(outs),
        scratch_shapes=[dma((len(outs),))],
        compiler_params=pltpu.CompilerParams(vmem_limit_bytes=4 * 1024 * 1024),
    )(*[pltpu.with_memory_space_constraint(a, pltpu.VMEM) for a in results])


def on_device(
    expert_input,
    cotangent,
    routes,
    route_weight,
    expert_gate,
    expert_up,
    expert_down,
    conv_out,
    conv_value,
    conv_gate,
    conv_taps,
    norm_gain,
    norm_bias,
    out_weight,
):
    big = (
        expert_input,
        cotangent,
        conv_out,
        expert_gate,
        expert_up,
        expert_down,
        out_weight,
        conv_value,
        conv_gate,
        conv_taps,
    )
    resid_grad, gate_grad, up_grad, down_grad, out_weight_grad, value_grad, gate_in_grad = run_step(
        routes.T,
        route_weight.T,
        norm_gain[None, :],
        norm_bias[None, :],
        big,
        lax.axis_size("sp"),
        lax.axis_size("tp"),
    )
    return (gate_grad, up_grad, down_grad, resid_grad, out_weight_grad, value_grad, gate_in_grad)


def solution(mesh):
    return jax.shard_map(
        on_device,
        mesh=mesh,
        in_specs=(
            P("sp", None),
            P("sp", None),
            P("sp", None),
            P("sp", None),
            P("sp", None, "tp"),
            P("sp", None, "tp"),
            P("sp", "tp", None),
            P("sp", "tp"),
            P("sp", "tp"),
            P("sp", "tp"),
            P(None, "tp"),
            P("tp"),
            P("tp"),
            P("tp", None),
        ),
        out_specs=(
            P("sp", None, "tp"),
            P("sp", None, "tp"),
            P("sp", "tp", None),
            P("sp", None),
            P("tp", "sp"),
            P("sp", "tp"),
            P("sp", "tp"),
        ),
        check_vma=False,
    )
```
